32 devices in a mesh: sp: 8 (over z, y), tp: 4 (over x, core).
Axes of the slice: x: 2, y: 2, z: 4, core: 2. Of those that a mesh axis runs over, the one named last changes fastest.
Arguments:
- query_rows: bfloat16 [2048, 2048], P('sp', 'tp'), may hold values from -5.5 to 5.5
- key_rows: bfloat16 [2048, 2048], P('sp', 'tp'), may hold values from -5.5 to 5.5
- value_rows: bfloat16 [2048, 2048], P('sp', 'tp'), may hold values from -6 to 6
- out_grad: bfloat16 [2048, 2048], P('sp', 'tp'), may hold values from -96 to 96
- rel_bias: float32 [256, 32], replicated, may hold values from -3 to 3
Outputs:
- query_grad: bfloat16 [2048, 2048], P('sp', 'tp')
- key_grad: bfloat16 [2048, 2048], P('sp', 'tp')
- value_grad: bfloat16 [2048, 2048], P('sp', 'tp')
- table_grad: float32 [256, 32], P('sp')
The draws below stay inside these ranges and needn't reach their ends.
All inputs are finite; a program needn't handle non-finite values.
Results may differ from the reference program's by a relative error of at most 0.007.
Values may be sent and summed in bfloat16 or wider, within the bound.
A program may use at most 64 MiB of HBM per device.

```python
import jax
import jax.numpy as jnp
from jax import lax

HEADS = 32
HEAD_DIM = 64
SEG = 64
LEFT = 4
CLIP = 128
TOKENS = 2048
TABLE = 256


def drawn_pair(key):
    key_queries, key_keys = jax.random.split(jax.random.fold_in(key, 11), 2)
    width_all = HEADS * HEAD_DIM
    query_draw = jnp.clip(jax.random.normal(key_queries, (TOKENS, width_all), jnp.float32), -5.5, 5.5)
    key_draw = jnp.clip(jax.random.normal(key_keys, (TOKENS, width_all), jnp.float32), -5.5, 5.5)
    return (query_draw, key_draw)


def draw_query_rows(key, part):
    return drawn_pair(key)[0].astype(jnp.bfloat16)


def draw_key_rows(key, part):
    return drawn_pair(key)[1].astype(jnp.bfloat16)


def steps_of(rng, shape, shards, low, top_value):
    def one(dim, shards_of):
        draws = jax.random.uniform(jax.random.fold_in(jax.random.fold_in(rng, 6), dim), (shards_of,), jnp.float32, low / len(shards), top_value / len(shards))
        return jnp.repeat(jnp.exp(draws), shape[dim] // shards_of).reshape((-1,) + (1,) * (len(shape) - dim - 1))

    loudness = one(*shards[0])
    for cut in shards[1:]:
        loudness = loudness * one(*cut)
    return loudness


def gaussian(rng, dims, width, limit, pieces=(), kind=jnp.bfloat16):
    factor_of = steps_of(rng, dims, pieces, -0.22, 0.18) if pieces else 1.0
    drawn = jax.random.normal(rng, dims, jnp.float32) * width * factor_of
    return jnp.minimum(jnp.maximum(drawn, -limit), limit).astype(kind)


def setup_inputs(seed: int = 0) -> dict:
    key_of = jax.random.split(jax.random.key(seed), 6)
    return {
        "query_rows": draw_query_rows(jax.random.fold_in(key_of[5], 71), 0),
        "key_rows": draw_key_rows(jax.random.fold_in(key_of[5], 71), 0),
        "value_rows": gaussian(key_of[2], (TOKENS, HEADS * HEAD_DIM), 1.0, 6.0, ((0, 8), (1, 4))),
        "out_grad": gaussian(key_of[3], (TOKENS, HEADS * HEAD_DIM), 16.0, 96.0, ((0, 8), (1, 4))),
        "rel_bias": gaussian(key_of[4], (TABLE, HEADS), 0.5, 3.0, (), jnp.float32),
    }


NEG_FILL = -1e30


def banded(extended, seg_count, seg_len, band_len):
    layers = []
    for offset in range(band_len // seg_len):
        window = lax.slice_in_dim(extended, offset * seg_len, offset * seg_len + seg_count * seg_len, axis=0)
        layers.append(window.reshape((seg_count, 1, seg_len) + extended.shape[1:]))
    return jnp.concatenate(layers, axis=1).reshape((seg_count, band_len) + extended.shape[1:])


def unbanded(band_grads, ext_len, seg_len):
    seg_count, band_len = band_grads.shape[0], band_grads.shape[1]
    trailing = band_grads.shape[2:]
    blocks = band_grads.reshape((seg_count, band_len // seg_len, seg_len) + trailing)
    summed = jnp.zeros((ext_len,) + trailing, band_grads.dtype)
    for offset in range(band_len // seg_len):
        stripe = blocks[:, offset].reshape((seg_count * seg_len,) + trailing)
        widths = [(offset * seg_len, ext_len - offset * seg_len - seg_count * seg_len)] + [(0, 0)] * len(trailing)
        summed = summed + jnp.pad(stripe, widths)
    return summed


def head_backward(inputs):
    query_head, key_head, value_head, dout_head, table_col = inputs
    reach_rows = LEFT * SEG
    band_len = reach_rows + SEG
    seg_count = TOKENS // SEG
    score_scale = HEAD_DIM ** -0.5
    key_ext = jnp.pad(key_head.astype(jnp.float32), ((reach_rows, 0), (0, 0)))
    value_ext = jnp.pad(value_head.astype(jnp.float32), ((reach_rows, 0), (0, 0)))
    key_valid = jnp.arange(reach_rows + TOKENS, dtype=jnp.int32) >= reach_rows
    key_band = banded(key_ext, seg_count, SEG, band_len)
    value_band = banded(value_ext, seg_count, SEG, band_len)
    valid_band = banded(key_valid, seg_count, SEG, band_len)
    query_segs = query_head.astype(jnp.float32).reshape(seg_count, SEG, HEAD_DIM)
    dout_segs = dout_head.astype(jnp.float32).reshape(seg_count, SEG, HEAD_DIM)
    row_pos = jnp.arange(SEG, dtype=jnp.int32)[:, None]
    col_pos = jnp.arange(band_len, dtype=jnp.int32)[None, :]
    offset_index = jnp.clip(reach_rows + row_pos - col_pos, -CLIP, CLIP - 1) + CLIP
    bias_band = table_col[offset_index]
    scores = jnp.einsum('jid,jcd->jic', query_segs, key_band) * score_scale + bias_band[None]
    scores = jnp.where(valid_band[:, None, :], scores, NEG_FILL)
    row_peak = jnp.max(scores, axis=-1)
    log_norm = row_peak + jnp.log(jnp.sum(jnp.exp(scores - row_peak[..., None]), axis=-1))
    attention = jnp.exp(scores - log_norm[..., None])
    attention_half = lax.optimization_barrier(attention.astype(jnp.bfloat16)).astype(jnp.float32)
    attention_grad = jnp.einsum('jie,jce->jic', dout_segs, value_band)
    inner_sums = jnp.sum(attention * attention_grad, axis=-1)
    dscores = attention * (attention_grad - inner_sums[..., None])
    dscore_half = lax.optimization_barrier(dscores.astype(jnp.bfloat16)).astype(jnp.float32)
    dquery = (jnp.einsum('jic,jcd->jid', dscore_half, key_band) * score_scale).reshape(TOKENS, HEAD_DIM)
    dkey_band = jnp.einsum('jic,jid->jcd', dscore_half, query_segs) * score_scale
    dvalue_band = jnp.einsum('jic,jie->jce', attention_half, dout_segs)
    key_grad_rows = unbanded(dkey_band, reach_rows + TOKENS, SEG)[reach_rows:]
    value_grad_rows = unbanded(dvalue_band, reach_rows + TOKENS, SEG)[reach_rows:]
    table_col_grad = jax.ops.segment_sum(jnp.sum(dscores, axis=0).reshape(-1), offset_index.reshape(-1), num_segments=2 * CLIP)
    return dquery.astype(jnp.bfloat16), key_grad_rows.astype(jnp.bfloat16), value_grad_rows.astype(jnp.bfloat16), table_col_grad


def split_heads(row_block):
    return jnp.transpose(row_block.reshape(TOKENS, HEADS, HEAD_DIM), (1, 0, 2))


def join_heads(stacked):
    return jnp.transpose(stacked, (1, 0, 2)).reshape(TOKENS, HEADS * HEAD_DIM)


def reference(query_rows, key_rows, value_rows, out_grad, rel_bias):
    results = lax.map(head_backward, (split_heads(query_rows), split_heads(key_rows), split_heads(value_rows), split_heads(out_grad), jnp.transpose(rel_bias)))
    return (join_heads(results[0]), join_heads(results[1]), join_heads(results[2]), jnp.transpose(results[3]))
```

```python
from functools import partial
import math

import jax
import jax.numpy as jnp
from jax import lax
from jax.experimental import pallas as pl
from jax.experimental.pallas import tpu as pltpu
from jax.sharding import PartitionSpec as P

HEAD_DIM = 64
SEG = 64
LEFT = 4
CLIP = 128

LANES = 2 * HEAD_DIM
REACH = LEFT * SEG
BLK = 2 * SEG
BAND = REACH + BLK
WRAP = 3 * BLK
NEG_FILL = -1e30
LOG2E = math.log2(math.e)
MESH = pl.DeviceIdType.MESH
F32 = jnp.float32
BF16 = jnp.bfloat16

NT = (((1,), (1,)), ((), ()))
NN = (((1,), (0,)), ((), ()))
TN = (((0,), (0,)), ((), ()))


def dot(a, b, dims):
    return lax.dot_general(a, b, dims, preferred_element_type=F32)


def turned(x, amount):
    amount %= x.shape[1]
    return pltpu.roll(x, amount, 1) if amount else x


def row_turned(x, sign):
    row = lax.broadcasted_iota(jnp.int32, x.shape, 0)
    for bit in (1, 2, 4):
        x = jnp.where((row & bit) != 0, turned(x, sign * bit), x)
    return x


def build_bias(table_row, first, bias_ref, pair, lane):
    last = table_row[:, 2 * CLIP - 1 :]
    flat = jnp.broadcast_to(last, (1, BLK))
    shape = (8, BLK)
    line = jnp.concatenate([table_row[:, CLIP:], flat, table_row[:, :CLIP]], axis=1)
    base = row_turned(jnp.broadcast_to(line, (8, WRAP)), 1)
    query = lax.broadcasted_iota(jnp.int32, shape, 1)
    wall = jnp.where(first, NEG_FILL, 0.0)
    cols = pl.ds(lane * BLK, BLK)
    flat8 = jnp.broadcast_to(last, shape)
    for group in range(BAND // 8):
        row = group * 8
        if row < BLK:
            tile = flat8
        else:
            sheared = turned(base, row % BLK)
            tile = sheared[:, BLK : 2 * BLK] if row < 2 * BLK else sheared[:, :BLK]
        if row < SEG:
            tile = jnp.where(query >= SEG, NEG_FILL, tile)
        if row >= BAND - SEG:
            tile = jnp.where(query < SEG, NEG_FILL, tile)
        bias_ref[pair, 0, pl.ds(row, 8), cols] = tile + wall if row < REACH else tile
        bias_ref[pair, 1, pl.ds(row, 8), cols] = tile + wall if row < REACH - BLK else tile


def diagonals(square):
    parts = []
    for group in range(BLK // 8):
        near = square[2 * BLK + group * 8 : 2 * BLK + group * 8 + 8]
        far = square[BLK + group * 8 : BLK + group * 8 + 8]
        parts.append(jnp.concatenate([near, far, jnp.zeros_like(near)], axis=1))
    step = 8
    while len(parts) > 1:
        parts = [a + turned(b, -step) for a, b in zip(parts[::2], parts[1::2])]
        step *= 2
    sums = jnp.sum(row_turned(parts[0], -1), axis=0, keepdims=True)
    return sums, jnp.sum(square[:BLK], axis=0, keepdims=True)


def kernel(
    sp_size, tp_size,
    q_hbm, k_hbm, v_hbm, d_hbm, table_ref,
    dq_ref, dk_ref, dv_ref, dt_ref,
    q_ref, d_ref, kx, vx, bias_ref, square_ref,
    own_k, own_v, back_k, back_v, got_k, got_v,
    table_rows, pieces, piece_got, shares,
    load_sem, halo_send, halo_recv, back_send, back_recv,
    piece_send, piece_recv, share_send, share_recv,
):
    rows, width = q_hbm.shape
    pairs = width // LANES
    heads = width // HEAD_DIM
    me = lax.axis_index("sp")
    col = lax.axis_index("tp")
    has_left = me > 0
    has_right = me < sp_size - 1
    left = jnp.maximum(me - 1, 0)
    right = jnp.minimum(me + 1, sp_size - 1)

    own = pl.ds(REACH, rows)
    loads = [
        pltpu.make_async_copy(src, dst, load_sem.at[i])
        for i, (src, dst) in enumerate(
            ((k_hbm, kx.at[own]), (v_hbm, vx.at[own]), (q_hbm, q_ref), (d_hbm, d_ref))
        )
    ]
    for load in loads:
        load.start()

    barrier = pltpu.get_barrier_semaphore()
    for k in range(1, sp_size):
        pl.semaphore_signal(
            barrier, inc=1, device_id=(lax.rem(me + k, sp_size), col), device_id_type=MESH
        )
    for k in range(1, tp_size):
        pl.semaphore_signal(
            barrier, inc=1, device_id=(me, lax.rem(col + k, tp_size)), device_id_type=MESH
        )
    pl.semaphore_wait(barrier, sp_size - 1 + tp_size - 1)

    def halo_copies(p):
        cols = pl.ds(p * LANES, LANES)
        return [
            pltpu.make_async_remote_copy(
                src_ref=src.at[:, cols],
                dst_ref=dst.at[pl.ds(0, REACH), cols],
                send_sem=halo_send.at[p, i],
                recv_sem=halo_recv.at[p, i],
                device_id=(right, col),
                device_id_type=MESH,
            )
            for i, (src, dst) in enumerate(((k_hbm, kx), (v_hbm, vx)))
        ]

    def back_copies(p):
        return [
            pltpu.make_async_remote_copy(
                src_ref=src.at[p],
                dst_ref=dst.at[p],
                send_sem=back_send.at[p, i],
                recv_sem=back_recv.at[p, i],
                device_id=(left, col),
                device_id_type=MESH,
            )
            for i, (src, dst) in enumerate(((back_k, got_k), (back_v, got_v)))
        ]

    @pl.when(has_right)
    def _():
        for p in range(pairs):
            for copy in halo_copies(p):
                copy.start()

    @pl.when(jnp.logical_not(has_left))
    def _():
        kx[0:REACH, :] = jnp.zeros((REACH, width), BF16)
        vx[0:REACH, :] = jnp.zeros((REACH, width), BF16)

    table_rows[...] = jnp.transpose(table_ref[...]) * LOG2E
    for h in range(heads):
        row = table_rows[pl.ds(col * heads + h, 1), :]
        build_bias(row, jnp.logical_not(has_left), bias_ref, h // 2, h % 2)

    for load in loads:
        load.wait()

    low = lax.broadcasted_iota(jnp.int32, (BLK, LANES), 1) < HEAD_DIM
    scale = HEAD_DIM ** -0.5
    sums, tops = [], []

    def split(x):
        zero = jnp.zeros_like(x)
        return jnp.concatenate([jnp.where(low, x, zero), jnp.where(low, zero, x)], axis=0)

    for p in range(pairs):
        cols = pl.ds(p * LANES, LANES)

        @pl.when(has_left)
        def _():
            for copy in halo_copies(p):
                copy.wait_recv()

        grads = []
        for half in range(2):
            keys = pl.ds(half * BLK, BAND)
            mine = pl.ds(half * BLK, BLK)
            k_blk = kx[keys, cols]
            v_blk = vx[keys, cols]
            qq = split(q_ref[mine, cols] * jnp.asarray(scale, BF16))
            dd = split(d_ref[mine, cols])
            scores = dot(k_blk, qq, NT) * LOG2E + bias_ref[p, half]
            dprobs = dot(v_blk, dd, NT)
            peak = jnp.max(scores, axis=0, keepdims=True)
            grown = jnp.exp2(scores - peak)
            inverse = 1.0 / jnp.sum(grown, axis=0, keepdims=True)
            probs = grown * inverse
            inner = jnp.sum(probs * dprobs, axis=0, keepdims=True)
            dscores = probs * (dprobs - inner)
            if half == 0:
                square_ref[...] = dscores
            else:
                square_ref[...] += dscores
            ds_half = dscores.astype(BF16)
            grads.append((dot(ds_half, qq, NN), dot(probs.astype(BF16), dd, NN)))
            flat = dot(k_blk, ds_half, TN)
            both = jnp.concatenate([flat[:HEAD_DIM, :BLK], flat[HEAD_DIM:, BLK:]], axis=0)
            dq_ref[mine, cols] = (jnp.transpose(both) * scale).astype(BF16)
        for i, (back, mine_ref) in enumerate(((back_k, own_k), (back_v, own_v))):
            a, b = grads[0][i], grads[1][i]
            back[p, 0:BLK, :] = a[:BLK].astype(BF16)
            back[p, BLK:REACH, :] = (a[BLK:REACH] + b[: REACH - BLK]).astype(BF16)
            mine_ref[p, 0:BLK, :] = a[REACH:] + b[REACH - BLK : REACH]
            mine_ref[p, BLK:rows, :] = b[REACH:]

        @pl.when(has_left)
        def _():
            for copy in back_copies(p):
                copy.start()

        for lane in range(2):
            s, t = diagonals(square_ref[:, lane * BLK : (lane + 1) * BLK])
            sums.append(s)
            tops.append(t)

    y = jnp.concatenate(sums, axis=0)
    beyond = jnp.sum(
        y[:, BLK : 2 * BLK] + jnp.concatenate(tops, axis=0), axis=1, keepdims=True
    )
    spot = lax.broadcasted_iota(jnp.int32, (heads, BLK), 1)
    upper = y[:, :BLK] + jnp.where(spot == BLK - 1, beyond, 0.0)
    grad_rows = jnp.concatenate([y[:, 2 * BLK :], upper], axis=1)
    part = 2 * CLIP // sp_size
    for s in range(sp_size):
        pieces[s] = turned(grad_rows, -part * s)[:, :BLK]

    def piece_copy(k):
        target = lax.rem(me + k, sp_size)
        return pltpu.make_async_remote_copy(
            src_ref=pieces.at[target],
            dst_ref=piece_got.at[k - 1],
            send_sem=piece_send.at[k - 1],
            recv_sem=piece_recv.at[k - 1],
            device_id=(target, col),
            device_id_type=MESH,
        )

    def share_copy(k):
        return pltpu.make_async_remote_copy(
            src_ref=shares.at[col],
            dst_ref=shares.at[col],
            send_sem=share_send.at[k - 1],
            recv_sem=share_recv.at[k - 1],
            device_id=(me, lax.rem(col + k, tp_size)),
            device_id_type=MESH,
        )

    def share_arrival(k):
        source = lax.rem(col + tp_size - k, tp_size)
        return pltpu.make_async_remote_copy(
            src_ref=shares.at[source],
            dst_ref=shares.at[source],
            send_sem=share_send.at[k - 1],
            recv_sem=share_recv.at[k - 1],
            device_id=(me, source),
            device_id_type=MESH,
        )

    for k in range(1, sp_size):
        piece_copy(k).start()

    def finish(p):
        cols = pl.ds(p * LANES, LANES)

        @pl.when(has_right)
        def _():
            for copy in back_copies(p):
                copy.wait_recv()
            dk_ref[:, cols] = (own_k[p] + got_k[p].astype(F32)).astype(BF16)
            dv_ref[:, cols] = (own_v[p] + got_v[p].astype(F32)).astype(BF16)

        @pl.when(jnp.logical_not(has_right))
        def _():
            dk_ref[:, cols] = own_k[p].astype(BF16)
            dv_ref[:, cols] = own_v[p].astype(BF16)

    total = pieces[me]
    for k in range(1, sp_size):
        piece_copy(k).wait_recv()
        total = total + piece_got[k - 1]
    shares[col] = total
    for k in range(1, tp_size):
        share_copy(k).start()
    for p in range(pairs):
        finish(p)
    for k in range(1, tp_size):
        share_arrival(k).wait_recv()
    stacked = jnp.concatenate([shares[t] for t in range(tp_size)], axis=0)
    dt_ref[...] = jnp.transpose(stacked)[:part]

    for k in range(1, sp_size):
        piece_copy(k).wait_send()
    for k in range(1, tp_size):
        share_copy(k).wait_send()

    @pl.when(has_right)
    def _():
        for p in range(pairs):
            for copy in halo_copies(p):
                copy.wait_send()

    @pl.when(has_left)
    def _():
        for p in range(pairs):
            for copy in back_copies(p):
                copy.wait_send()


def shards(sp_size, tp_size, query_rows, key_rows, value_rows, out_grad, rel_bias):
    rows, width = query_rows.shape
    pairs = width // LANES
    heads = width // HEAD_DIM
    part = 2 * CLIP // sp_size
    assert rows == REACH and REACH == 2 * BLK and CLIP == BLK
    like = jax.ShapeDtypeStruct((rows, width), BF16)
    dma = pltpu.SemaphoreType.DMA
    return pl.pallas_call(
        partial(kernel, sp_size, tp_size),
        out_shape=(like, like, like, jax.ShapeDtypeStruct((part, heads * tp_size), F32)),
        in_specs=[pl.BlockSpec(memory_space=pl.ANY)] * 4
        + [pl.BlockSpec(memory_space=pltpu.VMEM)],
        out_specs=tuple([pl.BlockSpec(memory_space=pltpu.VMEM)] * 4),
        scratch_shapes=[
            pltpu.VMEM((rows, width), BF16),
            pltpu.VMEM((rows, width), BF16),
            pltpu.VMEM((REACH + rows, width), BF16),
            pltpu.VMEM((REACH + rows, width), BF16),
            pltpu.VMEM((pairs, 2, BAND, 2 * BLK), F32),
            pltpu.VMEM((BAND, 2 * BLK), F32),
            pltpu.VMEM((pairs, rows, LANES), F32),
            pltpu.VMEM((pairs, rows, LANES), F32),
            pltpu.VMEM((pairs, REACH, LANES), BF16),
            pltpu.VMEM((pairs, REACH, LANES), BF16),
            pltpu.VMEM((pairs, REACH, LANES), BF16),
            pltpu.VMEM((pairs, REACH, LANES), BF16),
            pltpu.VMEM(rel_bias.shape[::-1], F32),
            pltpu.VMEM((sp_size, heads, BLK), F32),
            pltpu.VMEM((sp_size - 1, heads, BLK), F32),
            pltpu.VMEM((tp_size, heads, BLK), F32),
            dma((4,)),
            dma((pairs, 2)),
            dma((pairs, 2)),
            dma((pairs, 2)),
            dma((pairs, 2)),
            dma((sp_size - 1,)),
            dma((sp_size - 1,)),
            dma((tp_size - 1,)),
            dma((tp_size - 1,)),
        ],
        compiler_params=pltpu.CompilerParams(
            collective_id=0, has_side_effects=True, vmem_limit_bytes=48 * 1024 * 1024
        ),
    )(query_rows, key_rows, value_rows, out_grad, rel_bias)


def solution(mesh):
    return jax.shard_map(
        partial(shards, mesh.shape["sp"], mesh.shape["tp"]),
        mesh=mesh,
        in_specs=(P("sp", "tp"), P("sp", "tp"), P("sp", "tp"), P("sp", "tp"), P()),
        out_specs=(P("sp", "tp"), P("sp", "tp"), P("sp", "tp"), P("sp", None)),
        check_vma=False,
    )
```

```python
from functools import partial
import math

import jax
import jax.numpy as jnp
from jax import lax
from jax.experimental import pallas as pl
from jax.experimental.pallas import tpu as pltpu
from jax.sharding import PartitionSpec as P

HEAD_DIM = 64
SEG = 64
LEFT = 4
CLIP = 128

LANES = 2 * HEAD_DIM
REACH = LEFT * SEG
BLK = 2 * SEG
BAND = REACH + BLK
WRAP = 3 * BLK
NEG_FILL = -1e30
LOG2E = math.log2(math.e)
MESH = pl.DeviceIdType.MESH
F32 = jnp.float32
BF16 = jnp.bfloat16

NT = (((1,), (1,)), ((), ()))
NN = (((1,), (0,)), ((), ()))
TN = (((0,), (0,)), ((), ()))


def dot(a, b, dims):
    return lax.dot_general(a, b, dims, preferred_element_type=F32)


def turned(x, amount):
    amount %= x.shape[1]
    return pltpu.roll(x, amount, 1) if amount else x


def row_turned(x, sign):
    row = lax.broadcasted_iota(jnp.int32, x.shape, 0)
    for bit in (1, 2, 4):
        x = jnp.where((row & bit) != 0, turned(x, sign * bit), x)
    return x


def build_bias(table_row, first, bias_ref, pair, lane):
    last = table_row[:, 2 * CLIP - 1 :]
    flat = jnp.broadcast_to(last, (1, BLK))
    shape = (8, BLK)
    line = jnp.concatenate([table_row[:, CLIP:], flat, table_row[:, :CLIP]], axis=1)
    base = row_turned(jnp.broadcast_to(line, (8, WRAP)), 1)
    query = lax.broadcasted_iota(jnp.int32, shape, 1)
    wall = jnp.where(first, NEG_FILL, 0.0)
    cols = pl.ds(lane * BLK, BLK)
    flat8 = jnp.broadcast_to(last, shape)
    for group in range(BAND // 8):
        row = group * 8
        if row < BLK:
            tile = flat8
        else:
            sheared = turned(base, row % BLK)
            tile = sheared[:, BLK : 2 * BLK] if row < 2 * BLK else sheared[:, :BLK]
        if row < SEG:
            tile = jnp.where(query >= SEG, NEG_FILL, tile)
        if row >= BAND - SEG:
            tile = jnp.where(query < SEG, NEG_FILL, tile)
        bias_ref[pair, 0, pl.ds(row, 8), cols] = tile + wall if row < REACH else tile
        bias_ref[pair, 1, pl.ds(row, 8), cols] = tile + wall if row < REACH - BLK else tile


def diagonals(square):
    parts = []
    for group in range(BLK // 8):
        near = square[2 * BLK + group * 8 : 2 * BLK + group * 8 + 8]
        far = square[BLK + group * 8 : BLK + group * 8 + 8]
        parts.append(jnp.concatenate([near, far, jnp.zeros_like(near)], axis=1))
    step = 8
    while len(parts) > 1:
        parts = [a + turned(b, -step) for a, b in zip(parts[::2], parts[1::2])]
        step *= 2
    sums = jnp.sum(row_turned(parts[0], -1), axis=0, keepdims=True)
    return sums, jnp.sum(square[:BLK], axis=0, keepdims=True)


def kernel(
    sp_size, tp_size,
    q_hbm, k_hbm, v_hbm, d_hbm, table_hbm,
    dq_ref, dk_ref, dv_ref, dt_ref,
    q_ref, d_ref, kx, vx, bias_ref, square_ref,
    own_k, own_v, back_k, back_v, got_k, got_v,
    table_rows, pieces, piece_got, shares,
    load_sem, halo_send, halo_recv, back_send, back_recv,
    piece_send, piece_recv, share_send, share_recv,
):
    rows, width = q_hbm.shape
    pairs = width // LANES
    heads = width // HEAD_DIM
    me = lax.axis_index("sp")
    col = lax.axis_index("tp")
    has_left = me > 0
    has_right = me < sp_size - 1
    left = jnp.maximum(me - 1, 0)
    right = jnp.minimum(me + 1, sp_size - 1)

    own = pl.ds(REACH, rows)
    loads = [
        pltpu.make_async_copy(src, dst, load_sem.at[i])
        for i, (src, dst) in enumerate(
            (
                (k_hbm, kx.at[own]),
                (v_hbm, vx.at[own]),
                (q_hbm, q_ref),
                (d_hbm, d_ref),
                (table_hbm, table_rows),
            )
        )
    ]
    for load in loads:
        load.start()

    barrier = pltpu.get_barrier_semaphore()
    for k in range(1, sp_size):
        pl.semaphore_signal(
            barrier, inc=1, device_id=(lax.rem(me + k, sp_size), col), device_id_type=MESH
        )
    for k in range(1, tp_size):
        pl.semaphore_signal(
            barrier, inc=1, device_id=(me, lax.rem(col + k, tp_size)), device_id_type=MESH
        )
    pl.semaphore_wait(barrier, sp_size - 1 + tp_size - 1)

    def halo_copies(p):
        cols = pl.ds(p * LANES, LANES)
        return [
            pltpu.make_async_remote_copy(
                src_ref=src.at[:, cols],
                dst_ref=dst.at[pl.ds(0, REACH), cols],
                send_sem=halo_send.at[p, i],
                recv_sem=halo_recv.at[p, i],
                device_id=(right, col),
                device_id_type=MESH,
            )
            for i, (src, dst) in enumerate(((k_hbm, kx), (v_hbm, vx)))
        ]

    def back_copies(p):
        return [
            pltpu.make_async_remote_copy(
                src_ref=src.at[p],
                dst_ref=dst.at[p],
                send_sem=back_send.at[p, i],
                recv_sem=back_recv.at[p, i],
                device_id=(left, col),
                device_id_type=MESH,
            )
            for i, (src, dst) in enumerate(((back_k, got_k), (back_v, got_v)))
        ]

    def send_back(p):
        @pl.when(has_left)
        def _():
            for copy in back_copies(p):
                copy.start()

    @pl.when(has_right)
    def _():
        for p in range(pairs):
            for copy in halo_copies(p):
                copy.start()

    @pl.when(jnp.logical_not(has_left))
    def _():
        kx[0:REACH, :] = jnp.zeros((REACH, width), BF16)
        vx[0:REACH, :] = jnp.zeros((REACH, width), BF16)

    loads[4].wait()
    for h in range(heads):
        row = table_rows[pl.ds(col * heads + h, 1), :] * LOG2E
        build_bias(row, jnp.logical_not(has_left), bias_ref, h // 2, h % 2)

    for load in loads[:4]:
        load.wait()

    low = lax.broadcasted_iota(jnp.int32, (BLK, LANES), 1) < HEAD_DIM
    scale = HEAD_DIM ** -0.5
    sums, tops = [], []
    held = pairs

    def split(x):
        zero = jnp.zeros_like(x)
        return jnp.concatenate([jnp.where(low, x, zero), jnp.where(low, zero, x)], axis=0)

    for p in range(pairs):
        cols = pl.ds(p * LANES, LANES)

        @pl.when(has_left)
        def _():
            for copy in halo_copies(p):
                copy.wait_recv()

        grads = []
        for half in range(2):
            keys = pl.ds(half * BLK, BAND)
            mine = pl.ds(half * BLK, BLK)
            k_blk = kx[keys, cols]
            v_blk = vx[keys, cols]
            qq = split(q_ref[mine, cols] * jnp.asarray(scale, BF16))
            dd = split(d_ref[mine, cols])
            scores = dot(k_blk, qq, NT) * LOG2E + bias_ref[p, half]
            dprobs = dot(v_blk, dd, NT)
            peak = jnp.max(scores, axis=0, keepdims=True)
            grown = jnp.exp2(scores - peak)
            inverse = 1.0 / jnp.sum(grown, axis=0, keepdims=True)
            probs = grown * inverse
            inner = jnp.sum(probs * dprobs, axis=0, keepdims=True)
            dscores = probs * (dprobs - inner)
            if half == 0:
                square_ref[...] = dscores
            else:
                square_ref[...] += dscores
            ds_half = dscores.astype(BF16)
            grads.append((dot(ds_half, qq, NN), dot(probs.astype(BF16), dd, NN)))
            flat = dot(k_blk, ds_half, TN)
            both = jnp.concatenate([flat[:HEAD_DIM, :BLK], flat[HEAD_DIM:, BLK:]], axis=0)
            dq_ref[mine, cols] = (jnp.transpose(both) * scale).astype(BF16)
        for i, (back, mine_ref) in enumerate(((back_k, own_k), (back_v, own_v))):
            a, b = grads[0][i], grads[1][i]
            back[p, 0:BLK, :] = a[:BLK].astype(BF16)
            back[p, BLK:REACH, :] = (a[BLK:REACH] + b[: REACH - BLK]).astype(BF16)
            mine_ref[p, 0:BLK, :] = a[REACH:] + b[REACH - BLK : REACH]
            mine_ref[p, BLK:rows, :] = b[REACH:]

        if p < pairs - held:
            send_back(p)
        for lane in range(2):
            s, t = diagonals(square_ref[:, lane * BLK : (lane + 1) * BLK])
            sums.append(s)
            tops.append(t)

    y = jnp.concatenate(sums, axis=0)
    beyond = jnp.sum(
        y[:, BLK : 2 * BLK] + jnp.concatenate(tops, axis=0), axis=1, keepdims=True
    )
    spot = lax.broadcasted_iota(jnp.int32, (heads, BLK), 1)
    upper = y[:, :BLK] + jnp.where(spot == BLK - 1, beyond, 0.0)
    grad_rows = jnp.concatenate([y[:, 2 * BLK :], upper], axis=1)
    part = 2 * CLIP // sp_size
    for s in range(sp_size):
        pieces[s] = turned(grad_rows, -part * s)[:, :BLK]

    def piece_copy(k):
        target = lax.rem(me + k, sp_size)
        return pltpu.make_async_remote_copy(
            src_ref=pieces.at[target],
            dst_ref=piece_got.at[k - 1],
            send_sem=piece_send.at[k - 1],
            recv_sem=piece_recv.at[k - 1],
            device_id=(target, col),
            device_id_type=MESH,
        )

    def share_copy(k):
        return pltpu.make_async_remote_copy(
            src_ref=shares.at[col],
            dst_ref=shares.at[col],
            send_sem=share_send.at[k - 1],
            recv_sem=share_recv.at[k - 1],
            device_id=(me, lax.rem(col + k, tp_size)),
            device_id_type=MESH,
        )

    def share_arrival(k):
        source = lax.rem(col + tp_size - k, tp_size)
        return pltpu.make_async_remote_copy(
            src_ref=shares.at[source],
            dst_ref=shares.at[source],
            send_sem=share_send.at[k - 1],
            recv_sem=share_recv.at[k - 1],
            device_id=(me, source),
            device_id_type=MESH,
        )

    for k in range(1, sp_size):
        piece_copy(k).start()
    for p in range(pairs - held, pairs):
        send_back(p)

    def finish(p):
        cols = pl.ds(p * LANES, LANES)

        @pl.when(has_right)
        def _():
            for copy in back_copies(p):
                copy.wait_recv()
            dk_ref[:, cols] = (own_k[p] + got_k[p].astype(F32)).astype(BF16)
            dv_ref[:, cols] = (own_v[p] + got_v[p].astype(F32)).astype(BF16)

        @pl.when(jnp.logical_not(has_right))
        def _():
            dk_ref[:, cols] = own_k[p].astype(BF16)
            dv_ref[:, cols] = own_v[p].astype(BF16)

    total = pieces[me]
    for k in range(1, sp_size):
        piece_copy(k).wait_recv()
        total = total + piece_got[k - 1]
    shares[col] = total
    for k in range(1, tp_size):
        share_copy(k).start()
    for p in range(pairs):
        finish(p)
    for k in range(1, tp_size):
        share_arrival(k).wait_recv()
    stacked = jnp.concatenate([shares[t] for t in range(tp_size)], axis=0)
    dt_ref[...] = jnp.transpose(stacked)[:part]

    for k in range(1, sp_size):
        piece_copy(k).wait_send()
    for k in range(1, tp_size):
        share_copy(k).wait_send()

    @pl.when(has_right)
    def _():
        for p in range(pairs):
            for copy in halo_copies(p):
                copy.wait_send()

    @pl.when(has_left)
    def _():
        for p in range(pairs):
            for copy in back_copies(p):
                copy.wait_send()


def shards(sp_size, tp_size, query_rows, key_rows, value_rows, out_grad, rel_bias):
    rows, width = query_rows.shape
    pairs = width // LANES
    heads = width // HEAD_DIM
    part = 2 * CLIP // sp_size
    assert rows == REACH and REACH == 2 * BLK and CLIP == BLK
    like = jax.ShapeDtypeStruct((rows, width), BF16)
    dma = pltpu.SemaphoreType.DMA
    shapes = (like, like, like, jax.ShapeDtypeStruct((part, heads * tp_size), F32))
    results = pl.pallas_call(
        partial(kernel, sp_size, tp_size),
        out_shape=shapes,
        in_specs=[pl.BlockSpec(memory_space=pltpu.HBM)] * 5,
        out_specs=tuple([pl.BlockSpec(memory_space=pltpu.VMEM)] * 4),
        scratch_shapes=[
            pltpu.VMEM((rows, width), BF16),
            pltpu.VMEM((rows, width), BF16),
            pltpu.VMEM((REACH + rows, width), BF16),
            pltpu.VMEM((REACH + rows, width), BF16),
            pltpu.VMEM((pairs, 2, BAND, 2 * BLK), F32),
            pltpu.VMEM((BAND, 2 * BLK), F32),
            pltpu.VMEM((pairs, rows, LANES), F32),
            pltpu.VMEM((pairs, rows, LANES), F32),
            pltpu.VMEM((pairs, REACH, LANES), BF16),
            pltpu.VMEM((pairs, REACH, LANES), BF16),
            pltpu.VMEM((pairs, REACH, LANES), BF16),
            pltpu.VMEM((pairs, REACH, LANES), BF16),
            pltpu.VMEM(rel_bias.shape[::-1], F32),
            pltpu.VMEM((sp_size, heads, BLK), F32),
            pltpu.VMEM((sp_size - 1, heads, BLK), F32),
            pltpu.VMEM((tp_size, heads, BLK), F32),
            dma((5,)),
            dma((pairs, 2)),
            dma((pairs, 2)),
            dma((pairs, 2)),
            dma((pairs, 2)),
            dma((sp_size - 1,)),
            dma((sp_size - 1,)),
            dma((tp_size - 1,)),
            dma((tp_size - 1,)),
        ],
        compiler_params=pltpu.CompilerParams(
            collective_id=0, has_side_effects=True, vmem_limit_bytes=48 * 1024 * 1024
        ),
    )(*[pltpu.with_memory_space_constraint(x, pltpu.HBM) for x in (query_rows, key_rows, value_rows, out_grad, jnp.transpose(rel_bias))])
    return pl.pallas_call(
        write_out,
        out_shape=shapes,
        in_specs=[pl.BlockSpec(memory_space=pl.ANY)] * 4,
        out_specs=tuple([pl.BlockSpec(memory_space=pltpu.HBM)] * 4),
        scratch_shapes=[dma((4,))],
        compiler_params=pltpu.CompilerParams(vmem_limit_bytes=1024 * 1024),
    )(*results)


def write_out(*refs):
    sem = refs[-1]
    copies = [pltpu.make_async_copy(refs[i], refs[4 + i], sem.at[i]) for i in range(4)]
    for copy in copies:
        copy.start()
    for copy in copies:
        copy.wait()


def solution(mesh):
    return jax.shard_map(
        partial(shards, mesh.shape["sp"], mesh.shape["tp"]),
        mesh=mesh,
        in_specs=(P("sp", "tp"), P("sp", "tp"), P("sp", "tp"), P("sp", "tp"), P()),
        out_specs=(P("sp", "tp"), P("sp", "tp"), P("sp", "tp"), P("sp", None)),
        check_vma=False,
    )
```

```python
from functools import partial
import math

import jax
import jax.numpy as jnp
from jax import lax
from jax.experimental import pallas as pl
from jax.experimental.pallas import tpu as pltpu
from jax.sharding import PartitionSpec as P

HEAD_DIM = 64
SEG = 64
LEFT = 4
CLIP = 128

LANES = 2 * HEAD_DIM
REACH = LEFT * SEG
BLK = 2 * SEG
BAND = REACH + BLK
WRAP = 3 * BLK
NEG_FILL = -1e30
LOG2E = math.log2(math.e)
MESH = pl.DeviceIdType.MESH
F32 = jnp.float32
BF16 = jnp.bfloat16

NT = (((1,), (1,)), ((), ()))
NN = (((1,), (0,)), ((), ()))
TN = (((0,), (0,)), ((), ()))


def dot(a, b, dims):
    return lax.dot_general(a, b, dims, preferred_element_type=F32)


def turned(x, amount):
    amount %= x.shape[1]
    return pltpu.roll(x, amount, 1) if amount else x


def row_turned(x, sign):
    row = lax.broadcasted_iota(jnp.int32, x.shape, 0)
    for bit in (1, 2, 4):
        x = jnp.where((row & bit) != 0, turned(x, sign * bit), x)
    return x


def build_bias(table_row, bias_ref, pair, lane):
    last = table_row[:, 2 * CLIP - 1 :]
    flat = jnp.broadcast_to(last, (1, BLK))
    shape = (8, BLK)
    line = jnp.concatenate([table_row[:, CLIP:], flat, table_row[:, :CLIP]], axis=1)
    base = row_turned(jnp.broadcast_to(line, (8, WRAP)), 1)
    query = lax.broadcasted_iota(jnp.int32, shape, 1)
    cols = pl.ds(lane * BLK, BLK)
    flat8 = jnp.broadcast_to(last, shape)
    for group in range(BAND // 8):
        row = group * 8
        if row < BLK:
            tile = flat8
        else:
            sheared = turned(base, row % BLK)
            tile = sheared[:, BLK : 2 * BLK] if row < 2 * BLK else sheared[:, :BLK]
        if row < SEG:
            tile = jnp.where(query >= SEG, NEG_FILL, tile)
        if row >= BAND - SEG:
            tile = jnp.where(query < SEG, NEG_FILL, tile)
        bias_ref[pair, pl.ds(row, 8), cols] = tile


def diagonals(square):
    parts = []
    for group in range(BLK // 8):
        near = square[2 * BLK + group * 8 : 2 * BLK + group * 8 + 8]
        far = square[BLK + group * 8 : BLK + group * 8 + 8]
        parts.append(jnp.concatenate([near, far, jnp.zeros_like(near)], axis=1))
    step = 8
    while len(parts) > 1:
        parts = [a + turned(b, -step) for a, b in zip(parts[::2], parts[1::2])]
        step *= 2
    sums = jnp.sum(row_turned(parts[0], -1), axis=0, keepdims=True)
    return sums, jnp.sum(square[:BLK], axis=0, keepdims=True)


def kernel(
    sp_size, tp_size,
    q_hbm, k_hbm, v_hbm, d_hbm, table_hbm,
    dq_ref, dk_ref, dv_ref, dt_ref,
    qx, dx, k_ref, v_ref, bias_ref, square_ref, grown_ref, dprob_ref,
    own_k, own_v, own_q, back_q, got_q,
    local_stats, right_stats, halo_stats, left_stats,
    table_rows, pieces, piece_got, shares,
    load_sem, seq_send, seq_recv, ls_send, ls_recv, hs_send, hs_recv, back_send, back_recv,
    piece_send, piece_recv, share_send, share_recv,
):
    rows, width = q_hbm.shape
    pairs = width // LANES
    heads = width // HEAD_DIM
    me = lax.axis_index("sp")
    col = lax.axis_index("tp")
    has_left = me > 0
    has_right = me < sp_size - 1
    left = jnp.maximum(me - 1, 0)
    right = jnp.minimum(me + 1, sp_size - 1)

    own = pl.ds(0, rows)
    loads = [
        pltpu.make_async_copy(src, dst, load_sem.at[i])
        for i, (src, dst) in enumerate(
            (
                (k_hbm, k_ref),
                (v_hbm, v_ref),
                (q_hbm, qx.at[own]),
                (d_hbm, dx.at[own]),
                (table_hbm, table_rows),
            )
        )
    ]
    for load in loads:
        load.start()

    barrier = pltpu.get_barrier_semaphore()
    for k in range(1, sp_size):
        pl.semaphore_signal(
            barrier, inc=1, device_id=(lax.rem(me + k, sp_size), col), device_id_type=MESH
        )
    for k in range(1, tp_size):
        pl.semaphore_signal(
            barrier, inc=1, device_id=(me, lax.rem(col + k, tp_size)), device_id_type=MESH
        )
    pl.semaphore_wait(barrier, sp_size - 1 + tp_size - 1)

    def remote(src, dst, send, recv, target):
        return pltpu.make_async_remote_copy(
            src_ref=src,
            dst_ref=dst,
            send_sem=send,
            recv_sem=recv,
            device_id=(target, col),
            device_id_type=MESH,
        )

    def seq_copies(p):
        cols = pl.ds(p * LANES, LANES)
        return [
            remote(
                src.at[:, cols],
                dst.at[pl.ds(rows, rows), cols],
                seq_send.at[p, i],
                seq_recv.at[p, i],
                left,
            )
            for i, (src, dst) in enumerate(((q_hbm, qx), (d_hbm, dx)))
        ]

    def local_copy():
        return remote(local_stats, right_stats, ls_send, ls_recv, left)

    def halo_copy(p):
        return remote(halo_stats.at[p], left_stats.at[p], hs_send.at[p], hs_recv.at[p], right)

    def back_copy(p):
        return remote(back_q.at[p], got_q.at[p], back_send.at[p], back_recv.at[p], right)

    early = (pairs + 1) // 2

    @pl.when(has_left)
    def _():
        for p in range(early):
            for copy in seq_copies(p):
                copy.start()

    local_stats[...] = jnp.zeros(local_stats.shape, F32)
    halo_stats[...] = jnp.zeros(halo_stats.shape, F32)

    @pl.when(jnp.logical_not(has_left))
    def _():
        spot = lax.broadcasted_iota(jnp.int32, left_stats.shape, 1)
        left_stats[...] = jnp.where((spot == 0) | (spot == 3), NEG_FILL, 0.0)

    loads[4].wait()
    for h in range(heads):
        row = table_rows[pl.ds(col * heads + h, 1), :] * LOG2E
        build_bias(row, bias_ref, h // 2, h % 2)

    for load in loads[:4]:
        load.wait()

    low = lax.broadcasted_iota(jnp.int32, (BLK, LANES), 1) < HEAD_DIM
    scale = HEAD_DIM ** -0.5
    sums, tops = [], []

    def split(x):
        zero = jnp.zeros_like(x)
        return jnp.concatenate([jnp.where(low, x, zero), jnp.where(low, zero, x)], axis=0)

    def tile(p, half, halo):
        cols = pl.ds(p * LANES, LANES)
        mine = pl.ds(half * BLK + (rows if halo else 0), BLK)
        start, size, row = (
            (half * BLK, REACH - half * BLK, 0)
            if halo
            else (0, (half + 1) * BLK, REACH - half * BLK)
        )
        keys = pl.ds(start, size)
        qq = split(qx[mine, cols] * jnp.asarray(scale, BF16))
        dd = split(dx[mine, cols])
        return k_ref[keys, cols], v_ref[keys, cols], qq, dd, pl.ds(row, size)

    def partial_softmax(p, half, halo, stats):
        k_blk, v_blk, qq, dd, band = tile(p, half, halo)
        scores = dot(k_blk, qq, NT) * LOG2E + bias_ref[p, band]
        dprobs = dot(v_blk, dd, NT)
        peak = jnp.max(scores, axis=0, keepdims=True)
        grown = jnp.exp2(scores - peak)
        three = (
            peak,
            jnp.sum(grown, axis=0, keepdims=True),
            jnp.sum(grown * dprobs, axis=0, keepdims=True),
        )
        for i, value in enumerate(three):
            stats[p, pl.ds(half * 3 + i, 1), :] = value
        return grown, dprobs

    def tile_grads(p, half, halo, grown, dprobs, stats, others):
        k_blk, v_blk, qq, dd, band = tile(p, half, halo)
        m1, l1, i1 = (stats[p, pl.ds(half * 3 + i, 1), :] for i in range(3))
        m2, l2, i2 = (others[p, pl.ds(half * 3 + i, 1), :] for i in range(3))
        peak = jnp.maximum(m1, m2)
        a1, a2 = jnp.exp2(m1 - peak), jnp.exp2(m2 - peak)
        inverse = 1.0 / (l1 * a1 + l2 * a2)
        inner = (i1 * a1 + i2 * a2) * inverse
        probs = grown * (a1 * inverse)
        dscores = probs * (dprobs - inner)
        ds_half = dscores.astype(BF16)
        flat = dot(k_blk, ds_half, TN)
        both = jnp.concatenate([flat[:HEAD_DIM, :BLK], flat[HEAD_DIM:, BLK:]], axis=0)
        return (
            dscores,
            dot(ds_half, qq, NN),
            dot(probs.astype(BF16), dd, NN),
            jnp.transpose(both) * scale,
        )

    places = (pl.ds(0, BLK), pl.ds(BLK, 2 * BLK))
    for p in range(pairs):
        for half in range(2):
            grown, dprobs = partial_softmax(p, half, False, local_stats)
            grown_ref[p, places[half], :] = grown
            dprob_ref[p, places[half], :] = dprobs

    @pl.when(has_left)
    def _():
        local_copy().start()
        for p in range(early, pairs):
            for copy in seq_copies(p):
                copy.start()

    def halo(p):
        @pl.when(has_right)
        def _():
            for copy in seq_copies(p):
                copy.wait_recv()
            kept = [partial_softmax(p, half, True, halo_stats) for half in range(2)]
            halo_copy(p).start()
            if p == 0:
                local_copy().wait_recv()
            (s0, k0, v0, q0), (s1, k1, v1, q1) = (
                tile_grads(p, half, True, *kept[half], halo_stats, right_stats)
                for half in range(2)
            )
            for ref, a, b in ((own_k, k0, k1), (own_v, v0, v1)):
                ref[p, :BLK, :] = a[:BLK]
                ref[p, BLK:, :] = a[BLK:] + b
            back_q[p, :BLK, :] = q0.astype(BF16)
            back_q[p, BLK:, :] = q1.astype(BF16)
            square_ref[p, :BLK, :] = s0[:BLK] + s1
            square_ref[p, BLK:REACH, :] = s0[BLK:]

        @pl.when(jnp.logical_not(has_right))
        def _():
            own_k[p] = jnp.zeros((rows, LANES), F32)
            own_v[p] = jnp.zeros((rows, LANES), F32)
            square_ref[p, :REACH, :] = jnp.zeros((REACH, 2 * BLK), F32)

    def local(p):
        cols = pl.ds(p * LANES, LANES)

        @pl.when(has_left)
        def _():
            halo_copy(p).wait_recv()

        (s0, k0, v0, q0), (s1, k1, v1, q1) = (
            tile_grads(
                p, half, False,
                grown_ref[p, places[half], :], dprob_ref[p, places[half], :],
                local_stats, left_stats,
            )
            for half in range(2)
        )
        square = jnp.concatenate(
            [
                square_ref[p, :BLK, :],
                square_ref[p, BLK:REACH, :] + s1[:BLK],
                s0 + s1[BLK:],
            ],
            axis=0,
        )
        for lane in range(2):
            s, t = diagonals(square[:, lane * BLK : (lane + 1) * BLK])
            sums.append(s)
            tops.append(t)
        for out, ref, a, b in ((dk_ref, own_k, k0, k1), (dv_ref, own_v, v0, v1)):
            out[:BLK, cols] = (ref[p, :BLK, :] + a + b[:BLK]).astype(BF16)
            out[BLK:, cols] = (ref[p, BLK:, :] + b[BLK:]).astype(BF16)
        own_q[p, :BLK, :] = q0
        own_q[p, BLK:, :] = q1

    lag = 1
    for p in range(pairs + lag):
        if p < pairs:
            halo(p)
        if p >= lag:
            local(p - lag)

    y = jnp.concatenate(sums, axis=0)
    beyond = jnp.sum(
        y[:, BLK : 2 * BLK] + jnp.concatenate(tops, axis=0), axis=1, keepdims=True
    )
    spot = lax.broadcasted_iota(jnp.int32, (heads, BLK), 1)
    upper = y[:, :BLK] + jnp.where(spot == BLK - 1, beyond, 0.0)
    grad_rows = jnp.concatenate([y[:, 2 * BLK :], upper], axis=1)
    part = 2 * CLIP // sp_size
    for s in range(sp_size):
        pieces[s] = turned(grad_rows, -part * s)[:, :BLK]

    def piece_copy(k):
        target = lax.rem(me + k, sp_size)
        return pltpu.make_async_remote_copy(
            src_ref=pieces.at[target],
            dst_ref=piece_got.at[k - 1],
            send_sem=piece_send.at[k - 1],
            recv_sem=piece_recv.at[k - 1],
            device_id=(target, col),
            device_id_type=MESH,
        )

    def share_copy(k):
        return pltpu.make_async_remote_copy(
            src_ref=shares.at[col],
            dst_ref=shares.at[col],
            send_sem=share_send.at[k - 1],
            recv_sem=share_recv.at[k - 1],
            device_id=(me, lax.rem(col + k, tp_size)),
            device_id_type=MESH,
        )

    def share_arrival(k):
        source = lax.rem(col + tp_size - k, tp_size)
        return pltpu.make_async_remote_copy(
            src_ref=shares.at[source],
            dst_ref=shares.at[source],
            send_sem=share_send.at[k - 1],
            recv_sem=share_recv.at[k - 1],
            device_id=(me, source),
            device_id_type=MESH,
        )

    for k in range(1, sp_size):
        piece_copy(k).start()

    @pl.when(has_right)
    def _():
        for p in range(pairs):
            back_copy(p).start()

    def finish(p):
        cols = pl.ds(p * LANES, LANES)

        @pl.when(has_left)
        def _():
            back_copy(p).wait_recv()
            dq_ref[:, cols] = (own_q[p] + got_q[p].astype(F32)).astype(BF16)

        @pl.when(jnp.logical_not(has_left))
        def _():
            dq_ref[:, cols] = own_q[p].astype(BF16)

    total = pieces[me]
    for k in range(1, sp_size):
        piece_copy(k).wait_recv()
        total = total + piece_got[k - 1]
    shares[col] = total
    for k in range(1, tp_size):
        share_copy(k).start()
    for p in range(pairs):
        finish(p)
    for k in range(1, tp_size):
        share_arrival(k).wait_recv()
    stacked = jnp.concatenate([shares[t] for t in range(tp_size)], axis=0)
    dt_ref[...] = jnp.transpose(stacked)[:part]

    for k in range(1, sp_size):
        piece_copy(k).wait_send()
    for k in range(1, tp_size):
        share_copy(k).wait_send()

    @pl.when(has_left)
    def _():
        local_copy().wait_send()
        for p in range(pairs):
            for copy in seq_copies(p):
                copy.wait_send()

    @pl.when(has_right)
    def _():
        for p in range(pairs):
            halo_copy(p).wait_send()
            back_copy(p).wait_send()


def shards(sp_size, tp_size, query_rows, key_rows, value_rows, out_grad, rel_bias):
    rows, width = query_rows.shape
    pairs = width // LANES
    heads = width // HEAD_DIM
    part = 2 * CLIP // sp_size
    assert rows == REACH and REACH == 2 * BLK and CLIP == BLK
    like = jax.ShapeDtypeStruct((rows, width), BF16)
    dma = pltpu.SemaphoreType.DMA
    shapes = (like, like, like, jax.ShapeDtypeStruct((part, heads * tp_size), F32))
    results = pl.pallas_call(
        partial(kernel, sp_size, tp_size),
        out_shape=shapes,
        in_specs=[pl.BlockSpec(memory_space=pltpu.HBM)] * 5,
        out_specs=tuple([pl.BlockSpec(memory_space=pltpu.VMEM)] * 4),
        scratch_shapes=[
            pltpu.VMEM((2 * rows, width), BF16),
            pltpu.VMEM((2 * rows, width), BF16),
            pltpu.VMEM((rows, width), BF16),
            pltpu.VMEM((rows, width), BF16),
            pltpu.VMEM((pairs, BAND, 2 * BLK), F32),
            pltpu.VMEM((pairs, REACH, 2 * BLK), F32),
            pltpu.VMEM((pairs, BAND, 2 * BLK), F32),
            pltpu.VMEM((pairs, BAND, 2 * BLK), F32),
            pltpu.VMEM((pairs, rows, LANES), F32),
            pltpu.VMEM((pairs, rows, LANES), F32),
            pltpu.VMEM((pairs, rows, LANES), F32),
            pltpu.VMEM((pairs, rows, LANES), BF16),
            pltpu.VMEM((pairs, rows, LANES), BF16),
            pltpu.VMEM((pairs, 8, 2 * BLK), F32),
            pltpu.VMEM((pairs, 8, 2 * BLK), F32),
            pltpu.VMEM((pairs, 8, 2 * BLK), F32),
            pltpu.VMEM((pairs, 8, 2 * BLK), F32),
            pltpu.VMEM(rel_bias.shape[::-1], F32),
            pltpu.VMEM((sp_size, heads, BLK), F32),
            pltpu.VMEM((sp_size - 1, heads, BLK), F32),
            pltpu.VMEM((tp_size, heads, BLK), F32),
            dma((5,)),
            dma((pairs, 2)),
            dma((pairs, 2)),
            dma,
            dma,
            dma((pairs,)),
            dma((pairs,)),
            dma((pairs,)),
            dma((pairs,)),
            dma((sp_size - 1,)),
            dma((sp_size - 1,)),
            dma((tp_size - 1,)),
            dma((tp_size - 1,)),
        ],
        compiler_params=pltpu.CompilerParams(
            collective_id=0, has_side_effects=True, vmem_limit_bytes=48 * 1024 * 1024
        ),
    )(*[pltpu.with_memory_space_constraint(x, pltpu.HBM) for x in (query_rows, key_rows, value_rows, out_grad, jnp.transpose(rel_bias))])
    return pl.pallas_call(
        write_out,
        out_shape=shapes,
        in_specs=[pl.BlockSpec(memory_space=pl.ANY)] * 4,
        out_specs=tuple([pl.BlockSpec(memory_space=pltpu.HBM)] * 4),
        scratch_shapes=[dma((4,))],
        compiler_params=pltpu.CompilerParams(vmem_limit_bytes=1024 * 1024),
    )(*results)


def write_out(*refs):
    sem = refs[-1]
    copies = [pltpu.make_async_copy(refs[i], refs[4 + i], sem.at[i]) for i in range(4)]
    for copy in copies:
        copy.start()
    for copy in copies:
        copy.wait()


def solution(mesh):
    return jax.shard_map(
        partial(shards, mesh.shape["sp"], mesh.shape["tp"]),
        mesh=mesh,
        in_specs=(P("sp", "tp"), P("sp", "tp"), P("sp", "tp"), P("sp", "tp"), P()),
        out_specs=(P("sp", "tp"), P("sp", "tp"), P("sp", "tp"), P("sp", None)),
        check_vma=False,
    )
```

```python
from functools import partial
import math

import jax
import jax.numpy as jnp
from jax import lax
from jax.experimental import pallas as pl
from jax.experimental.pallas import tpu as pltpu
from jax.sharding import PartitionSpec as P

HEAD_DIM = 64
SEG = 64
LEFT = 4
CLIP = 128

LANES = 2 * HEAD_DIM
REACH = LEFT * SEG
BLK = 2 * SEG
BAND = REACH + BLK
WRAP = 3 * BLK
NEG_FILL = -1e30
LOG2E = math.log2(math.e)
MESH = pl.DeviceIdType.MESH
F32 = jnp.float32
BF16 = jnp.bfloat16

NT = (((1,), (1,)), ((), ()))
NN = (((1,), (0,)), ((), ()))
TN = (((0,), (0,)), ((), ()))


def dot(a, b, dims):
    return lax.dot_general(a, b, dims, preferred_element_type=F32)


def turned(x, amount):
    amount %= x.shape[1]
    return pltpu.roll(x, amount, 1) if amount else x


def row_turned(x, sign):
    row = lax.broadcasted_iota(jnp.int32, x.shape, 0)
    for bit in (1, 2, 4):
        x = jnp.where((row & bit) != 0, turned(x, sign * bit), x)
    return x


def build_bias(table_row, bias_ref, pair, lane):
    last = table_row[:, 2 * CLIP - 1 :]
    flat = jnp.broadcast_to(last, (1, BLK))
    shape = (8, BLK)
    line = jnp.concatenate([table_row[:, CLIP:], flat, table_row[:, :CLIP]], axis=1)
    base = row_turned(jnp.broadcast_to(line, (8, WRAP)), 1)
    query = lax.broadcasted_iota(jnp.int32, shape, 1)
    cols = pl.ds(lane * BLK, BLK)
    flat8 = jnp.broadcast_to(last, shape)
    for group in range(BAND // 8):
        row = group * 8
        if row < BLK:
            tile = flat8
        else:
            sheared = turned(base, row % BLK)
            tile = sheared[:, BLK : 2 * BLK] if row < 2 * BLK else sheared[:, :BLK]
        if row < SEG:
            tile = jnp.where(query >= SEG, NEG_FILL, tile)
        if row >= BAND - SEG:
            tile = jnp.where(query < SEG, NEG_FILL, tile)
        bias_ref[pair, pl.ds(row, 8), cols] = tile


def diagonals(square):
    parts = []
    for group in range(BLK // 8):
        near = square[2 * BLK + group * 8 : 2 * BLK + group * 8 + 8]
        far = square[BLK + group * 8 : BLK + group * 8 + 8]
        parts.append(jnp.concatenate([near, far, jnp.zeros_like(near)], axis=1))
    step = 8
    while len(parts) > 1:
        parts = [a + turned(b, -step) for a, b in zip(parts[::2], parts[1::2])]
        step *= 2
    sums = jnp.sum(row_turned(parts[0], -1), axis=0, keepdims=True)
    return sums, jnp.sum(square[:BLK], axis=0, keepdims=True)


def kernel(
    sp_size, tp_size,
    q_hbm, k_hbm, v_hbm, d_hbm, table_hbm,
    dq_ref, dk_ref, dv_ref, dt_ref,
    qx, dx, k_ref, v_ref, bias_ref, square_ref, grown_ref, dprob_ref,
    own_k, own_v, own_q, back_q, got_q,
    local_stats, right_stats, halo_stats, left_stats,
    table_rows, pieces, piece_got, shares,
    load_sem, seq_send, seq_recv, ls_send, ls_recv, hs_send, hs_recv, back_send, back_recv,
    piece_send, piece_recv, share_send, share_recv,
):
    rows, width = q_hbm.shape
    pairs = width // LANES
    heads = width // HEAD_DIM
    me = lax.axis_index("sp")
    col = lax.axis_index("tp")
    has_left = me > 0
    has_right = me < sp_size - 1
    left = jnp.maximum(me - 1, 0)
    right = jnp.minimum(me + 1, sp_size - 1)

    own = pl.ds(0, rows)
    loads = [
        pltpu.make_async_copy(src, dst, load_sem.at[i])
        for i, (src, dst) in enumerate(
            (
                (k_hbm, k_ref),
                (v_hbm, v_ref),
                (q_hbm, qx.at[own]),
                (d_hbm, dx.at[own]),
                (table_hbm, table_rows),
            )
        )
    ]
    for load in loads:
        load.start()

    barrier = pltpu.get_barrier_semaphore()
    for k in range(1, sp_size):
        pl.semaphore_signal(
            barrier, inc=1, device_id=(lax.rem(me + k, sp_size), col), device_id_type=MESH
        )
    for k in range(1, tp_size):
        pl.semaphore_signal(
            barrier, inc=1, device_id=(me, lax.rem(col + k, tp_size)), device_id_type=MESH
        )
    pl.semaphore_wait(barrier, sp_size - 1 + tp_size - 1)

    def remote(src, dst, send, recv, target):
        return pltpu.make_async_remote_copy(
            src_ref=src,
            dst_ref=dst,
            send_sem=send,
            recv_sem=recv,
            device_id=(target, col),
            device_id_type=MESH,
        )

    def seq_copies(p):
        cols = pl.ds(p * LANES, LANES)
        return [
            remote(
                src.at[:, cols],
                dst.at[pl.ds(rows, rows), cols],
                seq_send.at[p, i],
                seq_recv.at[p, i],
                left,
            )
            for i, (src, dst) in enumerate(((q_hbm, qx), (d_hbm, dx)))
        ]

    def local_copy():
        return remote(local_stats, right_stats, ls_send, ls_recv, left)

    def halo_copy(p):
        return remote(halo_stats.at[p], left_stats.at[p], hs_send.at[p], hs_recv.at[p], right)

    def back_copy(p):
        return remote(back_q.at[p], got_q.at[p], back_send.at[p], back_recv.at[p], right)

    early = (pairs + 1) // 2

    @pl.when(has_left)
    def _():
        for p in range(early):
            for copy in seq_copies(p):
                copy.start()

    local_stats[...] = jnp.zeros(local_stats.shape, F32)
    halo_stats[...] = jnp.zeros(halo_stats.shape, F32)

    @pl.when(jnp.logical_not(has_left))
    def _():
        spot = lax.broadcasted_iota(jnp.int32, left_stats.shape, 1)
        left_stats[...] = jnp.where((spot == 0) | (spot == 3), NEG_FILL, 0.0)

    loads[4].wait()
    for h in range(heads):
        row = table_rows[pl.ds(col * heads + h, 1), :] * LOG2E
        build_bias(row, bias_ref, h // 2, h % 2)

    for load in loads[:4]:
        load.wait()

    low = lax.broadcasted_iota(jnp.int32, (BLK, LANES), 1) < HEAD_DIM
    scale = HEAD_DIM ** -0.5
    sums, tops = [], []

    def split(x):
        zero = jnp.zeros_like(x)
        return jnp.concatenate([jnp.where(low, x, zero), jnp.where(low, zero, x)], axis=0)

    def tile(p, half, halo):
        cols = pl.ds(p * LANES, LANES)
        mine = pl.ds(half * BLK + (rows if halo else 0), BLK)
        start, size, row = (
            (half * BLK, REACH - half * BLK, 0)
            if halo
            else (0, (half + 1) * BLK, REACH - half * BLK)
        )
        keys = pl.ds(start, size)
        qq = split(qx[mine, cols] * jnp.asarray(scale, BF16))
        dd = split(dx[mine, cols])
        return k_ref[keys, cols], v_ref[keys, cols], qq, dd, pl.ds(row, size)

    def partial_softmax(p, half, halo, stats):
        k_blk, v_blk, qq, dd, band = tile(p, half, halo)
        scores = dot(k_blk, qq, NT) * LOG2E + bias_ref[p, band]
        dprobs = dot(v_blk, dd, NT)
        peak = jnp.max(scores, axis=0, keepdims=True)
        grown = jnp.exp2(scores - peak)
        three = (
            peak,
            jnp.sum(grown, axis=0, keepdims=True),
            jnp.sum(grown * dprobs, axis=0, keepdims=True),
        )
        for i, value in enumerate(three):
            stats[p, pl.ds(half * 3 + i, 1), :] = value
        return grown, dprobs

    def tile_grads(p, half, halo, grown, dprobs, stats, others):
        k_blk, v_blk, qq, dd, band = tile(p, half, halo)
        m1, l1, i1 = (stats[p, pl.ds(half * 3 + i, 1), :] for i in range(3))
        m2, l2, i2 = (others[p, pl.ds(half * 3 + i, 1), :] for i in range(3))
        peak = jnp.maximum(m1, m2)
        a1, a2 = jnp.exp2(m1 - peak), jnp.exp2(m2 - peak)
        inverse = 1.0 / (l1 * a1 + l2 * a2)
        inner = (i1 * a1 + i2 * a2) * inverse
        probs = grown * (a1 * inverse)
        dscores = probs * (dprobs - inner)
        ds_half = dscores.astype(BF16)
        flat = dot(k_blk, ds_half, TN)
        both = jnp.concatenate([flat[:HEAD_DIM, :BLK], flat[HEAD_DIM:, BLK:]], axis=0)
        return (
            dscores,
            dot(ds_half, qq, NN),
            dot(probs.astype(BF16), dd, NN),
            jnp.transpose(both) * scale,
        )

    places = (pl.ds(0, BLK), pl.ds(BLK, 2 * BLK))
    for p in range(pairs):
        for half in range(2):
            grown, dprobs = partial_softmax(p, half, False, local_stats)
            grown_ref[p, places[half], :] = grown
            dprob_ref[p, places[half], :] = dprobs

    @pl.when(has_left)
    def _():
        local_copy().start()
        for p in range(early, pairs):
            for copy in seq_copies(p):
                copy.start()

    def halo(p):
        @pl.when(has_right)
        def _():
            for copy in seq_copies(p):
                copy.wait_recv()
            kept = [partial_softmax(p, half, True, halo_stats) for half in range(2)]
            halo_copy(p).start()
            if p == 0:
                local_copy().wait_recv()
            (s0, k0, v0, q0), (s1, k1, v1, q1) = (
                tile_grads(p, half, True, *kept[half], halo_stats, right_stats)
                for half in range(2)
            )
            for ref, a, b in ((own_k, k0, k1), (own_v, v0, v1)):
                ref[p, :BLK, :] = a[:BLK]
                ref[p, BLK:, :] = a[BLK:] + b
            back_q[p, :BLK, :] = q0.astype(BF16)
            back_q[p, BLK:, :] = q1.astype(BF16)
            square_ref[p, :BLK, :] = s0[:BLK] + s1
            square_ref[p, BLK:REACH, :] = s0[BLK:]

        @pl.when(jnp.logical_not(has_right))
        def _():
            own_k[p] = jnp.zeros((rows, LANES), F32)
            own_v[p] = jnp.zeros((rows, LANES), F32)
            square_ref[p, :REACH, :] = jnp.zeros((REACH, 2 * BLK), F32)

    def local(p):
        cols = pl.ds(p * LANES, LANES)

        @pl.when(has_left)
        def _():
            halo_copy(p).wait_recv()

        (s0, k0, v0, q0), (s1, k1, v1, q1) = (
            tile_grads(
                p, half, False,
                grown_ref[p, places[half], :], dprob_ref[p, places[half], :],
                local_stats, left_stats,
            )
            for half in range(2)
        )
        square = jnp.concatenate(
            [
                square_ref[p, :BLK, :],
                square_ref[p, BLK:REACH, :] + s1[:BLK],
                s0 + s1[BLK:],
            ],
            axis=0,
        )
        for lane in range(2):
            s, t = diagonals(square[:, lane * BLK : (lane + 1) * BLK])
            sums.append(s)
            tops.append(t)
        for out, ref, a, b in ((dk_ref, own_k, k0, k1), (dv_ref, own_v, v0, v1)):
            out[:BLK, cols] = (ref[p, :BLK, :] + a + b[:BLK]).astype(BF16)
            out[BLK:, cols] = (ref[p, BLK:, :] + b[BLK:]).astype(BF16)
        own_q[p, :BLK, :] = q0
        own_q[p, BLK:, :] = q1

    lag = pairs
    for p in range(pairs + lag):
        if p < pairs:
            halo(p)
        if p >= lag:
            local(p - lag)

    y = jnp.concatenate(sums, axis=0)
    beyond = jnp.sum(
        y[:, BLK : 2 * BLK] + jnp.concatenate(tops, axis=0), axis=1, keepdims=True
    )
    spot = lax.broadcasted_iota(jnp.int32, (heads, BLK), 1)
    upper = y[:, :BLK] + jnp.where(spot == BLK - 1, beyond, 0.0)
    grad_rows = jnp.concatenate([y[:, 2 * BLK :], upper], axis=1)
    part = 2 * CLIP // sp_size
    for s in range(sp_size):
        pieces[s] = turned(grad_rows, -part * s)[:, :BLK]

    def piece_copy(k):
        target = lax.rem(me + k, sp_size)
        return pltpu.make_async_remote_copy(
            src_ref=pieces.at[target],
            dst_ref=piece_got.at[k - 1],
            send_sem=piece_send.at[k - 1],
            recv_sem=piece_recv.at[k - 1],
            device_id=(target, col),
            device_id_type=MESH,
        )

    def share_copy(k):
        return pltpu.make_async_remote_copy(
            src_ref=shares.at[col],
            dst_ref=shares.at[col],
            send_sem=share_send.at[k - 1],
            recv_sem=share_recv.at[k - 1],
            device_id=(me, lax.rem(col + k, tp_size)),
            device_id_type=MESH,
        )

    def share_arrival(k):
        source = lax.rem(col + tp_size - k, tp_size)
        return pltpu.make_async_remote_copy(
            src_ref=shares.at[source],
            dst_ref=shares.at[source],
            send_sem=share_send.at[k - 1],
            recv_sem=share_recv.at[k - 1],
            device_id=(me, source),
            device_id_type=MESH,
        )

    for k in range(1, sp_size):
        piece_copy(k).start()

    @pl.when(has_right)
    def _():
        for p in range(pairs):
            back_copy(p).start()

    def finish(p):
        cols = pl.ds(p * LANES, LANES)

        @pl.when(has_left)
        def _():
            back_copy(p).wait_recv()
            dq_ref[:, cols] = (own_q[p] + got_q[p].astype(F32)).astype(BF16)

        @pl.when(jnp.logical_not(has_left))
        def _():
            dq_ref[:, cols] = own_q[p].astype(BF16)

    total = pieces[me]
    for k in range(1, sp_size):
        piece_copy(k).wait_recv()
        total = total + piece_got[k - 1]
    shares[col] = total
    for k in range(1, tp_size):
        share_copy(k).start()
    for p in range(pairs):
        finish(p)
    for k in range(1, tp_size):
        share_arrival(k).wait_recv()
    stacked = jnp.concatenate([shares[t] for t in range(tp_size)], axis=0)
    dt_ref[...] = jnp.transpose(stacked)[:part]

    for k in range(1, sp_size):
        piece_copy(k).wait_send()
    for k in range(1, tp_size):
        share_copy(k).wait_send()

    @pl.when(has_left)
    def _():
        local_copy().wait_send()
        for p in range(pairs):
            for copy in seq_copies(p):
                copy.wait_send()

    @pl.when(has_right)
    def _():
        for p in range(pairs):
            halo_copy(p).wait_send()
            back_copy(p).wait_send()


def shards(sp_size, tp_size, query_rows, key_rows, value_rows, out_grad, rel_bias):
    rows, width = query_rows.shape
    pairs = width // LANES
    heads = width // HEAD_DIM
    part = 2 * CLIP // sp_size
    assert rows == REACH and REACH == 2 * BLK and CLIP == BLK
    like = jax.ShapeDtypeStruct((rows, width), BF16)
    dma = pltpu.SemaphoreType.DMA
    shapes = (like, like, like, jax.ShapeDtypeStruct((part, heads * tp_size), F32))
    results = pl.pallas_call(
        partial(kernel, sp_size, tp_size),
        out_shape=shapes,
        in_specs=[pl.BlockSpec(memory_space=pltpu.HBM)] * 5,
        out_specs=tuple([pl.BlockSpec(memory_space=pltpu.VMEM)] * 4),
        scratch_shapes=[
            pltpu.VMEM((2 * rows, width), BF16),
            pltpu.VMEM((2 * rows, width), BF16),
            pltpu.VMEM((rows, width), BF16),
            pltpu.VMEM((rows, width), BF16),
            pltpu.VMEM((pairs, BAND, 2 * BLK), F32),
            pltpu.VMEM((pairs, REACH, 2 * BLK), F32),
            pltpu.VMEM((pairs, BAND, 2 * BLK), F32),
            pltpu.VMEM((pairs, BAND, 2 * BLK), F32),
            pltpu.VMEM((pairs, rows, LANES), F32),
            pltpu.VMEM((pairs, rows, LANES), F32),
            pltpu.VMEM((pairs, rows, LANES), F32),
            pltpu.VMEM((pairs, rows, LANES), BF16),
            pltpu.VMEM((pairs, rows, LANES), BF16),
            pltpu.VMEM((pairs, 8, 2 * BLK), F32),
            pltpu.VMEM((pairs, 8, 2 * BLK), F32),
            pltpu.VMEM((pairs, 8, 2 * BLK), F32),
            pltpu.VMEM((pairs, 8, 2 * BLK), F32),
            pltpu.VMEM(rel_bias.shape[::-1], F32),
            pltpu.VMEM((sp_size, heads, BLK), F32),
            pltpu.VMEM((sp_size - 1, heads, BLK), F32),
            pltpu.VMEM((tp_size, heads, BLK), F32),
            dma((5,)),
            dma((pairs, 2)),
            dma((pairs, 2)),
            dma,
            dma,
            dma((pairs,)),
            dma((pairs,)),
            dma((pairs,)),
            dma((pairs,)),
            dma((sp_size - 1,)),
            dma((sp_size - 1,)),
            dma((tp_size - 1,)),
            dma((tp_size - 1,)),
        ],
        compiler_params=pltpu.CompilerParams(
            collective_id=0, has_side_effects=True, vmem_limit_bytes=48 * 1024 * 1024
        ),
    )(*[pltpu.with_memory_space_constraint(x, pltpu.HBM) for x in (query_rows, key_rows, value_rows, out_grad, jnp.transpose(rel_bias))])
    return pl.pallas_call(
        write_out,
        out_shape=shapes,
        in_specs=[pl.BlockSpec(memory_space=pl.ANY)] * 4,
        out_specs=tuple([pl.BlockSpec(memory_space=pltpu.HBM)] * 4),
        scratch_shapes=[dma((4,))],
        compiler_params=pltpu.CompilerParams(vmem_limit_bytes=1024 * 1024),
    )(*results)


def write_out(*refs):
    sem = refs[-1]
    copies = [pltpu.make_async_copy(refs[i], refs[4 + i], sem.at[i]) for i in range(4)]
    for copy in copies:
        copy.start()
    for copy in copies:
        copy.wait()


def solution(mesh):
    return jax.shard_map(
        partial(shards, mesh.shape["sp"], mesh.shape["tp"]),
        mesh=mesh,
        in_specs=(P("sp", "tp"), P("sp", "tp"), P("sp", "tp"), P("sp", "tp"), P()),
        out_specs=(P("sp", "tp"), P("sp", "tp"), P("sp", "tp"), P("sp", None)),
        check_vma=False,
    )
```
